32 devices in a mesh: tp: 8 (over z, core), dp: 4 (over y, x).
Axes of the slice: x: 2, y: 2, z: 4, core: 2. Of those that a mesh axis runs over, the one named last changes fastest.
Arguments:
- incoming_embeddings: bfloat16 [24, 4096], P('tp', 'dp'), may hold values from -12 to 12
- rescale_factors: bfloat16 [2, 4096], P(None, 'dp'), may hold values from 0.099609375 to 1.8984375
- probe_lift: bfloat16 [2, 4096, 4096], P(None, 'dp', 'tp'), may hold values from -0.09375 to 0.09375
- address_lift: bfloat16 [2, 4096, 4096], P(None, 'dp', 'tp'), may hold values from -0.09375 to 0.09375
- forget_lift: bfloat16 [2, 4096, 4096], P(None, 'dp', 'tp'), may hold values from -0.09375 to 0.09375
- forget_shift: float32 [2, 4096], P(None, 'tp'), may hold values from -6 to 3
- surplus_fade: float32 [2, 24, 4096], P(None, 'dp', 'tp'), may hold values from -0.7 to 0
- content_lift: bfloat16 [2, 4096, 8192], P(None, 'dp', 'tp'), may hold values from -0.09375 to 0.09375
- filter_lift: bfloat16 [2, 4096, 8192], P(None, 'dp', 'tp'), may hold values from -0.09375 to 0.09375
- readback_lift: bfloat16 [2, 8192, 4096], P(None, 'tp', 'dp'), may hold values from -0.0625 to 0.0625
- memory_tensor: float32 [2, 24, 128, 8192], P(None, 'dp', None, 'tp'), may hold values from -6 to 6
Outputs:
- mixed: bfloat16 [24, 4096], P('tp', 'dp')
- new_state: float32 [2, 24, 128, 8192], P(None, 'dp', None, 'tp')
The draws below stay inside these ranges and needn't reach their ends.
All inputs are finite; a program needn't handle non-finite values.
Results may differ from the reference program's by a relative error of at most 0.0085.
Values may be sent and summed in bfloat16 or wider, within the bound.
A program may use at most 128 MiB of HBM per device.

```python
import math
import jax
import jax.numpy as jnp
from jax import lax

D = 4096
HEADS = 32
DK = 128
DV = 256
BLOCKS = 2
KW = 4096
VW = 8192
SEQS = 24


def draw_incoming_embeddings(key, part):
    first_key = jax.random.fold_in(jax.random.fold_in(key, 11), 0)
    col_scale = jnp.exp(jnp.linspace(math.log(0.5), math.log(2.5), D)).astype(jnp.float32)
    base_draw = jax.random.normal(first_key, (SEQS, D), jnp.float32)
    return jnp.clip(base_draw * col_scale, -12.0, 12.0).astype(jnp.bfloat16)


def draw_surplus_fade(key, part):
    first_key, second_key = jax.random.split(jax.random.fold_in(key, 23))
    hit_mask = jax.random.randint(first_key, (BLOCKS, SEQS, KW), 0, 8) == 0
    drop_size = jax.random.uniform(second_key, (BLOCKS, SEQS, KW), jnp.float32, -0.7, -0.22)
    return jnp.where(hit_mask, drop_size, 0.0).astype(jnp.float32)


def block_levels(own_key, dims, cuts, least, top_value):
    factor_of = 1.0
    for position, parts in cuts:
        draws = jax.random.uniform(jax.random.fold_in(jax.random.fold_in(own_key, 6), position), (parts,), jnp.float32, least / len(cuts), top_value / len(cuts))
        factor_of = factor_of * jnp.repeat(jnp.exp(draws), dims[position] // parts).reshape((-1,) + (1,) * (len(dims) - 1 - position))
    return factor_of


def normal_values(key, dims, width, bound, cuts=(), kind=jnp.bfloat16):
    gain = block_levels(key, dims, cuts, -0.22, 0.18) if cuts else 1.0
    array = jax.random.normal(key, dims, jnp.float32) * width * gain
    return jnp.minimum(jnp.maximum(array, -bound), bound).astype(kind)


def setup_inputs(seed: int = 0) -> dict:
    streams_of = jax.random.split(jax.random.key(seed), 12)
    return {
        "incoming_embeddings": draw_incoming_embeddings(jax.random.fold_in(streams_of[11], 71), 0),
        "rescale_factors": jnp.clip(1.0 + 0.18 * jax.random.normal(streams_of[1], (BLOCKS, D), jnp.float32), 0.099609375, 1.8984375).astype(jnp.bfloat16),
        "probe_lift": normal_values(streams_of[2], (BLOCKS, D, KW), D ** -0.5, 0.09375, ((1, 4), (2, 8))),
        "address_lift": normal_values(streams_of[3], (BLOCKS, D, KW), D ** -0.5, 0.09375, ((1, 4), (2, 8))),
        "forget_lift": normal_values(streams_of[4], (BLOCKS, D, KW), D ** -0.5, 0.09375, ((1, 4), (2, 8))),
        "forget_shift": jnp.clip(-6.0 + 9.0 * jax.random.uniform(streams_of[5], (BLOCKS, KW), jnp.float32) ** block_levels(streams_of[5], (BLOCKS, KW), ((1, 8),), -0.2, 0.2), -6.0, 3.0),
        "surplus_fade": draw_surplus_fade(jax.random.fold_in(streams_of[11], 71), 0),
        "content_lift": normal_values(streams_of[7], (BLOCKS, D, VW), D ** -0.5, 0.09375, ((1, 4), (2, 8))),
        "filter_lift": normal_values(streams_of[8], (BLOCKS, D, VW), D ** -0.5, 0.09375, ((1, 4), (2, 8))),
        "readback_lift": normal_values(streams_of[9], (BLOCKS, VW, D), VW ** -0.5, 0.0625, ((1, 8), (2, 4))),
        "memory_tensor": normal_values(streams_of[10], (BLOCKS, SEQS, DK, VW), 1.0, 6.0, ((1, 4), (3, 8)), jnp.float32),
    }


def reference(incoming_embeddings, rescale_factors, probe_lift, address_lift, forget_lift, forget_shift, surplus_fade, content_lift, filter_lift, readback_lift, memory_tensor):
    stream = incoming_embeddings
    collected = []
    seq_count = incoming_embeddings.shape[0]
    for layer_ordinal in range(BLOCKS):
        resid = stream.astype(jnp.float32)
        inv_rms = lax.rsqrt(lax.optimization_barrier(jnp.sum(resid * resid, axis=1, keepdims=True)) / D + 1e-06)
        hidden = (resid * rescale_factors[layer_ordinal].astype(jnp.float32)).astype(jnp.bfloat16)

        def linear_map_step(matrix):
            return inv_rms * jnp.dot(hidden, matrix[layer_ordinal], preferred_element_type=jnp.float32)
        queries = linear_map_step(probe_lift) * DK ** (-0.5)
        key_vals = linear_map_step(address_lift)
        values = linear_map_step(content_lift)
        gate_vals = linear_map_step(filter_lift)
        forget_rate_ln = jax.nn.log_sigmoid(linear_map_step(forget_lift) + forget_shift[layer_ordinal]) / 16.0 + surplus_fade[layer_ordinal]
        old_state = memory_tensor[layer_ordinal].reshape(seq_count, DK, HEADS, DV)
        decays = jnp.transpose(jnp.exp(forget_rate_ln).reshape(seq_count, HEADS, DK), (0, 2, 1))
        key_heads = key_vals.reshape(seq_count, HEADS, DK)
        value_heads = values.reshape(seq_count, HEADS, DV)
        fresh = old_state * decays[..., None] + jnp.einsum('shk,she->skhe', key_heads, value_heads, precision=lax.Precision.HIGHEST)
        readout = jnp.einsum('shk,skhe->she', queries.reshape(seq_count, HEADS, DK), fresh, precision=lax.Precision.HIGHEST).reshape(seq_count, VW)
        gated = (readout * jax.nn.silu(gate_vals)).astype(jnp.bfloat16)
        branch = jnp.dot(gated, readback_lift[layer_ordinal], preferred_element_type=jnp.float32)
        stream = (resid + branch).astype(jnp.bfloat16)
        collected.append(fresh.reshape(seq_count, DK, VW))
    return (stream, jnp.stack(collected))
```

```python
import functools

import jax
import jax.numpy as jnp
from jax import lax
from jax.experimental import pallas as pl
from jax.experimental.pallas import tpu as pltpu
from jax.sharding import PartitionSpec as P

DK = 128
BLOCKS = 2
SUB = 8
LANES = 128
LINK = jnp.bfloat16
F32 = jnp.float32


def kernel(
    n_tp, n_dp, x_hbm, gain_hbm, q_hbm, k_hbm, f_hbm, shift_hbm, fade_hbm, v_hbm, g_hbm, o_hbm, state_hbm,
    mixed_ref, out_hbm,
    gain, shift, fade, wq, wk, wf, wv, wg, wo, state,
    xg, hid, send_b, recv_b, cols, vals, readout, gated_all, part, send_e, recv_e,
    misc_sem, w_sem, out_sem, a_send, a_recv, b_send, b_recv, d_send, d_recv, e_send, e_recv,
):
    tp = lax.axis_index("tp")
    dp = lax.axis_index("dp")
    rows_tp = x_hbm.shape[0]
    depth = x_hbm.shape[1]
    kc = q_hbm.shape[2]
    vc = v_hbm.shape[2]
    seqs = state_hbm.shape[1]
    heads = kc // DK
    dv = vc // heads
    per = seqs // rows_tp
    pad = hid.shape[0] // n_dp
    model = depth * n_dp

    def peer_tp(o):
        return lax.rem(tp + o, n_tp)

    def peer_dp(o):
        return lax.rem(dp + o, n_dp)

    weights = [(f_hbm, wf), (k_hbm, wk), (q_hbm, wq), (v_hbm, wv), (g_hbm, wg), (o_hbm, wo), (state_hbm, state)]

    def load(b, i):
        src, dst = weights[i]
        return pltpu.make_async_copy(src.at[b], dst.at[b], w_sem.at[b, i])

    misc = [
        pltpu.make_async_copy(x_hbm, xg.at[0, tp], misc_sem.at[0]),
        pltpu.make_async_copy(gain_hbm, gain, misc_sem.at[1]),
        pltpu.make_async_copy(shift_hbm, shift, misc_sem.at[2]),
        pltpu.make_async_copy(fade_hbm, fade, misc_sem.at[3]),
    ]
    misc[0].start()
    misc[1].start()
    for i in range(5):
        load(0, i).start()
    misc[2].start()
    misc[3].start()

    barrier = pltpu.get_barrier_semaphore()
    for o in range(1, n_tp):
        pl.semaphore_signal(barrier, inc=1, device_id={"tp": peer_tp(o)}, device_id_type=pl.DeviceIdType.MESH)
    for o in range(1, n_dp):
        pl.semaphore_signal(barrier, inc=1, device_id={"dp": peer_dp(o)}, device_id_type=pl.DeviceIdType.MESH)
    hid[...] = jnp.zeros_like(hid)
    readout[...] = jnp.zeros_like(readout)
    misc[0].wait()
    misc[1].wait()
    pl.semaphore_wait(barrier, n_tp + n_dp - 2)

    def remote(src, dst, ss, rs, axis, target):
        return pltpu.make_async_remote_copy(
            src_ref=src, dst_ref=dst, send_sem=ss, recv_sem=rs,
            device_id={axis: target}, device_id_type=pl.DeviceIdType.MESH,
        )

    sent = []
    stored = []
    resid = None
    for b in range(BLOCKS):
        for o in range(1, n_tp):
            c = remote(xg.at[b, tp], xg.at[b, tp], a_send.at[b, o], a_recv.at[b, o], "tp", peer_tp(o))
            c.start()
            sent.append(c)
        if resid is None:
            resid = xg[b, tp].astype(F32)
        for o in range(1, n_tp):
            src = lax.rem(tp + n_tp - o, n_tp)
            remote(xg.at[b, src], xg.at[b, src], a_send.at[b, o], a_recv.at[b, o], "tp", src).wait_recv()
        for i in range(n_tp):
            at = pad * (i // per) + rows_tp * (i % per)
            hid[at:at + rows_tp, :] = xg[b, i].astype(F32)
        full = hid[...]
        squares = jnp.sum(full * full, axis=1, keepdims=True)
        hidden = (full * gain[b:b + 1, :].astype(F32)).astype(jnp.bfloat16)

        sq_hi = squares.astype(LINK).astype(F32)
        sq_lo = squares - sq_hi

        def put(value, at):
            for d in range(n_dp):
                send_b[b, d, :, at:at + value.shape[1]] = value[pad * d:pad * (d + 1)].astype(LINK)

        put(jnp.broadcast_to(sq_hi, (pad * n_dp, LANES)), 3 * kc)
        put(jnp.broadcast_to(sq_lo, (pad * n_dp, LANES)), 3 * kc + LANES)
        first = 3 * kc + 2 * LANES
        chunks = [(0, first, (0, 1, 2)), (first, vc, (3,)), (first + vc, vc, (4,))]
        for c, (start, width, members) in enumerate(chunks):
            at = start
            for m in members:
                load(b, m).wait()
                w = weights[m][1]
                put(jnp.dot(hidden, w[b], preferred_element_type=F32), at)
                at += w.shape[2]
            for o in range(1, n_dp):
                copy = remote(
                    send_b.at[b, peer_dp(o), :, pl.ds(start, width)],
                    recv_b.at[b, o - 1, :, pl.ds(start, width)],
                    b_send.at[b, c, o], b_recv.at[b, c, o], "dp", peer_dp(o),
                )
                copy.start()
                sent.append(copy)
            if b == 0 and c == 0:
                load(b, 6).start()
                load(b, 5).start()
        if b == 0:
            misc[2].wait()
            misc[3].wait()
        if b + 1 < BLOCKS:
            for i in (0, 1, 2, 3, 4, 6, 5):
                load(b + 1, i).start()

        def collect(c):
            start, width, _ = chunks[c]
            for o in range(1, n_dp):
                remote(
                    send_b.at[b, dp, :, pl.ds(start, width)],
                    recv_b.at[b, o - 1, :, pl.ds(start, width)],
                    b_send.at[b, c, o], b_recv.at[b, c, o], "dp", peer_dp(o),
                ).wait_recv()
            total = send_b[b, dp, :, start:start + width].astype(F32)
            for o in range(1, n_dp):
                total = total + recv_b[b, o - 1, :, start:start + width].astype(F32)
            return total

        got = collect(0)
        sq = got[:, 3 * kc:3 * kc + 1] + got[:, 3 * kc + LANES:3 * kc + LANES + 1]
        inv = lax.rsqrt(sq / model + 1e-06)
        pre = got[:, :kc] * inv + shift[b:b + 1, :]
        log_sig = jnp.minimum(pre, 0.0) - jnp.log(1.0 + jnp.exp(-jnp.abs(pre)))
        cols[0:pad, :] = jnp.zeros((pad, kc), F32)
        cols[0:seqs, :] = jnp.exp(log_sig[:seqs] / 16.0 + fade[b])
        cols[pad:2 * pad, :] = got[:, kc:2 * kc] * inv
        cols[2 * pad:3 * pad, :] = got[:, 2 * kc:3 * kc] * inv * DK ** (-0.5)
        load(b, 6).wait()
        vals[...] = collect(1) * inv

        for h in range(heads):
            turned = jnp.transpose(cols[:, h * DK:(h + 1) * DK])
            for s in range(seqs):
                dc = turned[:, s:s + 1]
                kcol = turned[:, pad + s:pad + s + 1]
                qc = turned[:, 2 * pad + s:2 * pad + s + 1]
                sl = slice(h * dv, (h + 1) * dv)
                fresh = state[b, s, :, sl] * dc + kcol * vals[s:s + 1, sl]
                state[b, s, :, sl] = fresh
                readout[s:s + 1, sl] = jnp.sum(fresh * qc, axis=0, keepdims=True)
            done = pltpu.make_async_copy(
                state.at[b, :, :, pl.ds(h * dv, dv)], out_hbm.at[b, :, :, pl.ds(h * dv, dv)], out_sem.at[b, h]
            )
            done.start()
            stored.append(done)

        gate = collect(2) * inv
        gated_all[b, dp] = (readout[...] * (gate / (1.0 + jnp.exp(-gate)))).astype(LINK)

        for o in range(1, n_dp):
            copy = remote(gated_all.at[b, dp], gated_all.at[b, dp], d_send.at[b, o], d_recv.at[b, o], "dp", peer_dp(o))
            copy.start()
            sent.append(copy)
        load(b, 5).wait()
        for o in range(1, n_dp):
            src = lax.rem(dp + n_dp - o, n_dp)
            remote(gated_all.at[b, src], gated_all.at[b, src], d_send.at[b, o], d_recv.at[b, o], "dp", src).wait_recv()
        gathered = gated_all[b].astype(F32).reshape(n_dp * pad, vc).astype(jnp.bfloat16)
        part[...] = jnp.dot(gathered, wo[b], preferred_element_type=F32)

        for i in range(n_tp):
            at = pad * (i // per) + rows_tp * (i % per)
            send_e[b, i] = part[at:at + rows_tp, :].astype(LINK)
        for o in range(1, n_tp):
            copy = remote(send_e.at[b, peer_tp(o)], recv_e.at[b, o - 1], e_send.at[b, o], e_recv.at[b, o], "tp", peer_tp(o))
            copy.start()
            sent.append(copy)
        total = send_e[b, tp].astype(F32)
        for o in range(1, n_tp):
            remote(send_e.at[b, tp], recv_e.at[b, o - 1], e_send.at[b, o], e_recv.at[b, o], "tp", peer_tp(o)).wait_recv()
            total = total + recv_e[b, o - 1].astype(F32)
        stream = (resid + total).astype(jnp.bfloat16)
        resid = stream.astype(F32)
        if b + 1 < BLOCKS:
            xg[b + 1, tp] = stream
        else:
            mixed_ref[...] = stream

    for c in sent:
        c.wait_send()
    for c in stored:
        c.wait()


def shards(n_tp, n_dp, x, gain, wq, wk, wf, shift, fade, wv, wg, wo, state):
    rows_tp, depth = x.shape
    kc = wq.shape[2]
    vc = wv.shape[2]
    seqs = state.shape[1]
    heads = kc // DK
    pad = -(-seqs // SUB) * SUB
    width = 3 * kc + 2 * LANES + 2 * vc
    vm = pltpu.VMEM
    dma = pltpu.SemaphoreType.DMA
    anyspec = pl.BlockSpec(memory_space=pl.ANY)
    return pl.pallas_call(
        functools.partial(kernel, n_tp, n_dp),
        out_shape=(
            jax.ShapeDtypeStruct(x.shape, x.dtype),
            jax.ShapeDtypeStruct(state.shape, state.dtype),
        ),
        in_specs=[anyspec] * 11,
        out_specs=(pl.BlockSpec(memory_space=pltpu.VMEM), anyspec),
        scratch_shapes=[
            vm(gain.shape, gain.dtype),
            vm(shift.shape, shift.dtype),
            vm(fade.shape, fade.dtype),
            vm(wq.shape, wq.dtype),
            vm(wk.shape, wk.dtype),
            vm(wf.shape, wf.dtype),
            vm(wv.shape, wv.dtype),
            vm(wg.shape, wg.dtype),
            vm(wo.shape, wo.dtype),
            vm(state.shape, state.dtype),
            vm((BLOCKS, n_tp, rows_tp, depth), x.dtype),
            vm((n_dp * pad, depth), F32),
            vm((BLOCKS, n_dp, pad, width), LINK),
            vm((BLOCKS, n_dp - 1, pad, width), LINK),
            vm((3 * pad, kc), F32),
            vm((pad, vc), F32),
            vm((pad, vc), F32),
            vm((BLOCKS, n_dp, pad, vc), LINK),
            vm((n_dp * pad, wo.shape[2]), F32),
            vm((BLOCKS, n_tp, rows_tp, depth), LINK),
            vm((BLOCKS, n_tp - 1, rows_tp, depth), LINK),
            dma((4,)),
            dma((BLOCKS, 7)),
            dma((BLOCKS, heads)),
            dma((BLOCKS, n_tp)),
            dma((BLOCKS, n_tp)),
            dma((BLOCKS, 3, n_dp)),
            dma((BLOCKS, 3, n_dp)),
            dma((BLOCKS, n_dp)),
            dma((BLOCKS, n_dp)),
            dma((BLOCKS, n_tp)),
            dma((BLOCKS, n_tp)),
        ],
        compiler_params=pltpu.CompilerParams(
            collective_id=0, has_side_effects=True, vmem_limit_bytes=60 * 1024 * 1024
        ),
        name="decode_step",
    )(x, gain, wq, wk, wf, shift, fade, wv, wg, wo, state)


def solution(mesh):
    in_specs = (
        P("tp", "dp"),
        P(None, "dp"),
        P(None, "dp", "tp"),
        P(None, "dp", "tp"),
        P(None, "dp", "tp"),
        P(None, "tp"),
        P(None, "dp", "tp"),
        P(None, "dp", "tp"),
        P(None, "dp", "tp"),
        P(None, "tp", "dp"),
        P(None, "dp", None, "tp"),
    )
    out_specs = (P("tp", "dp"), P(None, "dp", None, "tp"))
    body = functools.partial(shards, mesh.shape["tp"], mesh.shape["dp"])
    return jax.shard_map(body, mesh=mesh, in_specs=in_specs, out_specs=out_specs, check_vma=False)
```

```python
import functools

import jax
import jax.numpy as jnp
from jax import lax
from jax.experimental import pallas as pl
from jax.experimental.pallas import tpu as pltpu
from jax.sharding import PartitionSpec as P

DK = 128
BLOCKS = 2
VMEM_BYTES = 67043328
SUB = 8
LANES = 128
LINK = jnp.bfloat16
F32 = jnp.float32


def kernel(
    n_tp, n_dp, x_hbm, gain_hbm, q_hbm, k_hbm, f_hbm, shift_hbm, fade_hbm, v_hbm, g_hbm, o_hbm, state_hbm,
    mixed_ref, state,
    gain, shift, fade, wq, wk, wf, wv, wg, wo,
    xg, hid, send_b, recv_b, cols, vals, readout, gated_all, part, send_e, recv_e,
    misc_sem, w_sem, a_send, a_recv, b_send, b_recv, d_send, d_recv, e_send, e_recv,
):
    tp = lax.axis_index("tp")
    dp = lax.axis_index("dp")
    rows_tp = x_hbm.shape[0]
    depth = x_hbm.shape[1]
    kc = q_hbm.shape[2]
    vc = v_hbm.shape[2]
    seqs = state_hbm.shape[1]
    heads = kc // DK
    dv = vc // heads
    groups = 2 if heads % 2 == 0 else 1
    per = seqs // rows_tp
    pad = hid.shape[0] // n_dp
    model = depth * n_dp

    def peer_tp(o):
        return lax.rem(tp + o, n_tp)

    def peer_dp(o):
        return lax.rem(dp + o, n_dp)

    weights = [(f_hbm, wf), (k_hbm, wk), (q_hbm, wq), (v_hbm, wv), (g_hbm, wg), (o_hbm, wo), (state_hbm, state)]

    def load(b, i):
        src, dst = weights[i]
        return pltpu.make_async_copy(src.at[b], dst.at[b], w_sem.at[b, i])

    misc = [
        pltpu.make_async_copy(x_hbm, xg.at[0, tp], misc_sem.at[0]),
        pltpu.make_async_copy(gain_hbm, gain, misc_sem.at[1]),
        pltpu.make_async_copy(shift_hbm, shift, misc_sem.at[2]),
        pltpu.make_async_copy(fade_hbm, fade, misc_sem.at[3]),
    ]
    misc[0].start()
    misc[1].start()
    for i in range(5):
        load(0, i).start()
    misc[2].start()
    misc[3].start()

    barrier = pltpu.get_barrier_semaphore()
    for o in range(1, n_tp):
        pl.semaphore_signal(barrier, inc=1, device_id={"tp": peer_tp(o)}, device_id_type=pl.DeviceIdType.MESH)
    for o in range(1, n_dp):
        pl.semaphore_signal(barrier, inc=1, device_id={"dp": peer_dp(o)}, device_id_type=pl.DeviceIdType.MESH)
    hid[...] = jnp.zeros_like(hid)
    readout[...] = jnp.zeros_like(readout)
    cols[...] = jnp.zeros_like(cols)
    misc[0].wait()
    misc[1].wait()
    pl.semaphore_wait(barrier, n_tp + n_dp - 2)

    def remote(src, dst, ss, rs, axis, target):
        return pltpu.make_async_remote_copy(
            src_ref=src, dst_ref=dst, send_sem=ss, recv_sem=rs,
            device_id={axis: target}, device_id_type=pl.DeviceIdType.MESH,
        )

    sent = []
    resid = None
    for b in range(BLOCKS):
        for o in range(1, n_tp):
            c = remote(xg.at[b, tp], xg.at[b, tp], a_send.at[b, o], a_recv.at[b, o], "tp", peer_tp(o))
            c.start()
            sent.append(c)
        if resid is None:
            resid = xg[b, tp].astype(F32)
        for o in range(1, n_tp):
            src = lax.rem(tp + n_tp - o, n_tp)
            remote(xg.at[b, src], xg.at[b, src], a_send.at[b, o], a_recv.at[b, o], "tp", src).wait_recv()
        for i in range(n_tp):
            at = pad * (i // per) + rows_tp * (i % per)
            hid[at:at + rows_tp, :] = xg[b, i].astype(F32)
        full = hid[...]
        squares = jnp.sum(full * full, axis=1, keepdims=True)
        hidden = (full * gain[b:b + 1, :].astype(F32)).astype(jnp.bfloat16)

        sq_hi = squares.astype(LINK).astype(F32)
        sq_lo = squares - sq_hi

        def put(value, at):
            for d in range(n_dp):
                send_b[b, d, :, at:at + value.shape[1]] = value[pad * d:pad * (d + 1)].astype(LINK)

        chunks = []
        at = 0
        for g in range(groups + 1):
            start = at
            if g < groups:
                ks = slice(g * kc // groups, (g + 1) * kc // groups)
                vs = slice(g * vc // groups, (g + 1) * vc // groups)
                plan = [(0, ks), (1, ks), (2, ks), (3, vs)]
            else:
                plan = [(4, slice(0, vc))]
            for m, sl in plan:
                if g != 1 or groups == 1:
                    load(b, m).wait()
                put(jnp.dot(hidden, weights[m][1][b, :, sl], preferred_element_type=F32), at)
                at += sl.stop - sl.start
            if g == 0:
                put(jnp.broadcast_to(sq_hi, (pad * n_dp, LANES)), at)
                put(jnp.broadcast_to(sq_lo, (pad * n_dp, LANES)), at + LANES)
                at += 2 * LANES
            width = at - start
            c = g
            chunks.append((start, width))
            for o in range(1, n_dp):
                copy = remote(
                    send_b.at[b, peer_dp(o), :, pl.ds(start, width)],
                    recv_b.at[b, o - 1, :, pl.ds(start, width)],
                    b_send.at[b, c, o], b_recv.at[b, c, o], "dp", peer_dp(o),
                )
                copy.start()
                sent.append(copy)
            if b == 0 and c == 0:
                load(b, 6).start()
                load(b, 5).start()
        if b == 0:
            misc[2].wait()
            misc[3].wait()
        if b + 1 < BLOCKS:
            for i in (0, 1, 2, 3, 4, 6, 5):
                load(b + 1, i).start()

        def collect(c):
            start, width = chunks[c]
            for o in range(1, n_dp):
                remote(
                    send_b.at[b, dp, :, pl.ds(start, width)],
                    recv_b.at[b, o - 1, :, pl.ds(start, width)],
                    b_send.at[b, c, o], b_recv.at[b, c, o], "dp", peer_dp(o),
                ).wait_recv()
            total = send_b[b, dp, :, start:start + width].astype(F32)
            for o in range(1, n_dp):
                total = total + recv_b[b, o - 1, :, start:start + width].astype(F32)
            return total

        kw, vw = kc // groups, vc // groups
        for g in range(groups):
            got = collect(g)
            if g == 0:
                sq = got[:, 3 * kw + vw:3 * kw + vw + 1] + got[:, 3 * kw + vw + LANES:3 * kw + vw + LANES + 1]
                inv = lax.rsqrt(sq / model + 1e-06)
            k0, v0 = g * kw, g * vw
            pre = got[:, :kw] * inv + shift[b:b + 1, k0:k0 + kw]
            log_sig = jnp.minimum(pre, 0.0) - jnp.log(1.0 + jnp.exp(-jnp.abs(pre)))
            cols[0:seqs, k0:k0 + kw] = jnp.exp(log_sig[:seqs] / 16.0 + fade[:, b, k0:k0 + kw])
            cols[pad:2 * pad, k0:k0 + kw] = got[:, kw:2 * kw] * inv
            cols[2 * pad:3 * pad, k0:k0 + kw] = got[:, 2 * kw:3 * kw] * inv * DK ** (-0.5)
            vals[:, v0:v0 + vw] = got[:, 3 * kw:3 * kw + vw] * inv
            if g == 0:
                load(b, 6).wait()
            for h in range(g * heads // groups, (g + 1) * heads // groups):
                turned = jnp.transpose(cols[:, h * DK:(h + 1) * DK])
                for s in range(seqs):
                    dc = turned[:, s:s + 1]
                    kcol = turned[:, pad + s:pad + s + 1]
                    qc = turned[:, 2 * pad + s:2 * pad + s + 1]
                    sl = slice(h * dv, (h + 1) * dv)
                    fresh = state[b, s, :, sl] * dc + kcol * vals[s:s + 1, sl]
                    state[b, s, :, sl] = fresh
                    readout[s:s + 1, sl] = jnp.sum(fresh * qc, axis=0, keepdims=True)

        gate = collect(groups) * inv
        gated_all[b, dp] = (readout[...] * (gate / (1.0 + jnp.exp(-gate)))).astype(LINK)

        for o in range(1, n_dp):
            copy = remote(gated_all.at[b, dp], gated_all.at[b, dp], d_send.at[b, o], d_recv.at[b, o], "dp", peer_dp(o))
            copy.start()
            sent.append(copy)
        load(b, 5).wait()
        for o in range(1, n_dp):
            src = lax.rem(dp + n_dp - o, n_dp)
            remote(gated_all.at[b, src], gated_all.at[b, src], d_send.at[b, o], d_recv.at[b, o], "dp", src).wait_recv()
        gathered = gated_all[b].astype(F32).reshape(n_dp * pad, vc).astype(jnp.bfloat16)
        part[...] = jnp.dot(gathered, wo[b], preferred_element_type=F32)

        for i in range(n_tp):
            at = pad * (i // per) + rows_tp * (i % per)
            send_e[b, i] = part[at:at + rows_tp, :].astype(LINK)
        for o in range(1, n_tp):
            copy = remote(send_e.at[b, peer_tp(o)], recv_e.at[b, o - 1], e_send.at[b, o], e_recv.at[b, o], "tp", peer_tp(o))
            copy.start()
            sent.append(copy)
        total = send_e[b, tp].astype(F32)
        for o in range(1, n_tp):
            remote(send_e.at[b, tp], recv_e.at[b, o - 1], e_send.at[b, o], e_recv.at[b, o], "tp", peer_tp(o)).wait_recv()
            total = total + recv_e[b, o - 1].astype(F32)
        stream = (resid + total).astype(jnp.bfloat16)
        resid = stream.astype(F32)
        if b + 1 < BLOCKS:
            xg[b + 1, tp] = stream
        else:
            mixed_ref[...] = stream

    for c in sent:
        c.wait_send()


def store(mixed_vmem, state_vmem, mixed_hbm, state_hbm, sems):
    moves = [pltpu.make_async_copy(state_vmem.at[b], state_hbm.at[b], sems.at[b]) for b in range(BLOCKS)]
    moves.append(pltpu.make_async_copy(mixed_vmem, mixed_hbm, sems.at[BLOCKS]))
    for move in moves:
        move.start()
    for move in moves:
        move.wait()


def shards(n_tp, n_dp, x, gain, wq, wk, wf, shift, fade, wv, wg, wo, state):
    fade = jnp.swapaxes(fade, 0, 1)
    rows_tp, depth = x.shape
    kc = wq.shape[2]
    vc = wv.shape[2]
    seqs = state.shape[1]
    pad = -(-seqs // SUB) * SUB
    width = 3 * kc + 2 * LANES + 2 * vc
    vm = pltpu.VMEM
    dma = pltpu.SemaphoreType.DMA
    anyspec = pl.BlockSpec(memory_space=pl.ANY)
    mixed, fresh = pl.pallas_call(
        functools.partial(kernel, n_tp, n_dp),
        out_shape=(
            pltpu.VMEM(x.shape, x.dtype),
            pltpu.VMEM(state.shape, state.dtype),
        ),
        in_specs=[anyspec] * 11,
        out_specs=(pl.BlockSpec(memory_space=pltpu.VMEM), pl.BlockSpec(memory_space=pltpu.VMEM)),
        scratch_shapes=[
            vm(gain.shape, gain.dtype),
            vm(shift.shape, shift.dtype),
            vm(fade.shape, fade.dtype),
            vm(wq.shape, wq.dtype),
            vm(wk.shape, wk.dtype),
            vm(wf.shape, wf.dtype),
            vm(wv.shape, wv.dtype),
            vm(wg.shape, wg.dtype),
            vm(wo.shape, wo.dtype),
            vm((BLOCKS, n_tp, rows_tp, depth), x.dtype),
            vm((n_dp * pad, depth), F32),
            vm((BLOCKS, n_dp, pad, width), LINK),
            vm((BLOCKS, n_dp - 1, pad, width), LINK),
            vm((3 * pad, kc), F32),
            vm((pad, vc), F32),
            vm((pad, vc), F32),
            vm((BLOCKS, n_dp, pad, vc), LINK),
            vm((n_dp * pad, wo.shape[2]), F32),
            vm((BLOCKS, n_tp, rows_tp, depth), LINK),
            vm((BLOCKS, n_tp - 1, rows_tp, depth), LINK),
            dma((4,)),
            dma((BLOCKS, 7)),
            dma((BLOCKS, n_tp)),
            dma((BLOCKS, n_tp)),
            dma((BLOCKS, 3, n_dp)),
            dma((BLOCKS, 3, n_dp)),
            dma((BLOCKS, n_dp)),
            dma((BLOCKS, n_dp)),
            dma((BLOCKS, n_tp)),
            dma((BLOCKS, n_tp)),
        ],
        compiler_params=pltpu.CompilerParams(
            collective_id=0, has_side_effects=True, vmem_limit_bytes=VMEM_BYTES - state.size * 4 - (1 << 20)
        ),
        name="decode_step",
    )(x, gain, wq, wk, wf, shift, fade, wv, wg, wo, state)
    return pl.pallas_call(
        store,
        out_shape=(
            jax.ShapeDtypeStruct(x.shape, x.dtype),
            jax.ShapeDtypeStruct(state.shape, state.dtype),
        ),
        in_specs=[pl.BlockSpec(memory_space=pltpu.VMEM)] * 2,
        out_specs=(anyspec, anyspec),
        scratch_shapes=[dma((BLOCKS + 1,))],
        compiler_params=pltpu.CompilerParams(vmem_limit_bytes=1 << 20),
        name="store_results",
    )(
        pltpu.with_memory_space_constraint(mixed, pltpu.VMEM),
        pltpu.with_memory_space_constraint(fresh, pltpu.VMEM),
    )


def solution(mesh):
    in_specs = (
        P("tp", "dp"),
        P(None, "dp"),
        P(None, "dp", "tp"),
        P(None, "dp", "tp"),
        P(None, "dp", "tp"),
        P(None, "tp"),
        P(None, "dp", "tp"),
        P(None, "dp", "tp"),
        P(None, "dp", "tp"),
        P(None, "tp", "dp"),
        P(None, "dp", None, "tp"),
    )
    out_specs = (P("tp", "dp"), P(None, "dp", None, "tp"))
    body = functools.partial(shards, mesh.shape["tp"], mesh.shape["dp"])
    return jax.shard_map(body, mesh=mesh, in_specs=in_specs, out_specs=out_specs, check_vma=False)
```
